512 devices in a mesh: sp: 32 (over z, x), tp: 16 (over y, core).
Axes of the slice: x: 4, y: 8, z: 8, core: 2. Of those that a mesh axis runs over, the one named last changes fastest.
Arguments:
- tokens: bfloat16 [8192, 4096], P('sp', 'tp'), may hold values from -6 to 6
- norm_gain: float32 [2, 4096], replicated, may hold values from 0.1 to 1.9
- w_value: bfloat16 [2, 4096, 2048], P(None, 'sp', 'tp'), may hold values from -0.09375 to 0.09375
- w_gate: bfloat16 [2, 4096, 2048], P(None, 'sp', 'tp'), may hold values from -0.09375 to 0.09375
- conv_taps: float32 [2, 31, 2048], P(None, None, 'tp'), may hold values from -3 to 3
- conv_bias: float32 [2, 2048], P(None, 'tp'), may hold values from -3 to 3
- chan_gain: float32 [2, 2048], P(None, 'tp'), may hold values from 0.1 to 1.9
- chan_bias: float32 [2, 2048], P(None, 'tp'), may hold values from -3 to 3
- w_out: bfloat16 [2, 2048, 4096], P(None, 'sp', 'tp'), may hold values from -0.125 to 0.125
Outputs:
- stream: bfloat16 [8192, 4096], P('sp', 'tp')
The draws below stay inside these ranges and needn't reach their ends.
All inputs are finite; a program needn't handle non-finite values.
Results may differ from the reference program's by a relative error of at most 0.011.
Values may be sent and summed in bfloat16 or wider, within the bound.
No kernel may reach another device: no remote copies, remote signals or barrier semaphores. Data moves between devices by JAX's collectives and lax.ppermute only.
A program may use at most 64 MiB of HBM per device.

```python
import jax
import jax.numpy as jnp
from jax import lax

D = 4096
C = 2048
K = 31
LAYERS = 2
TOKENS = 8192


def draw_conv_taps(key, part):
    first, second = jax.random.split(jax.random.fold_in(key, 7))
    base = jax.random.normal(first, (LAYERS, K, C), jnp.float32)
    factor = jnp.exp(jax.random.uniform(second, (LAYERS, 1, 32), jnp.float32, -1.1, 1.1))
    factor = jnp.repeat(factor, C // 32, axis=2)
    return jnp.clip(base * factor * K ** (-0.5), -3.0, 3.0)


def steps_of(own_key, dims, pieces, low, top_value):
    gain = 1.0
    for axis_at, parts in pieces:
        draws = jax.random.uniform(jax.random.fold_in(jax.random.fold_in(own_key, 6), axis_at), (parts,), jnp.float32, low / len(pieces), top_value / len(pieces))
        gain = gain * jnp.repeat(jnp.exp(draws), dims[axis_at] // parts).reshape((-1,) + (1,) * (len(dims) - 1 - axis_at))
    return gain


def centred(key, shape, scale, reach, pieces=(), kind=jnp.bfloat16):
    drawn = scale * jax.random.normal(key, shape, jnp.float32)
    if pieces:
        drawn = drawn * steps_of(key, shape, pieces, -0.22, 0.18)
    return jnp.clip(drawn, -reach, reach).astype(kind)


def setup_inputs(seed: int = 0) -> dict:
    key_list = jax.random.split(jax.random.key(seed), 10)
    tokens = centred(key_list[0], (TOKENS, D), 1.0, 6.0, ((0, 32), (1, 16)))
    norm_gain = jnp.clip(1.0 + 0.18 * jax.random.normal(key_list[1], (LAYERS, D), jnp.float32), 0.1, 1.9)
    w_value = centred(key_list[2], (LAYERS, D, C), D ** -0.5, 0.09375, ((1, 32), (2, 16)))
    w_gate = centred(key_list[3], (LAYERS, D, C), D ** -0.5, 0.09375, ((1, 32), (2, 16)))
    conv_taps = draw_conv_taps(jax.random.fold_in(key_list[9], 71), 0)
    conv_bias = centred(key_list[5], (LAYERS, C), 0.5, 3.0, ((1, 16),), jnp.float32)
    chan_gain = jnp.clip(1.0 + 0.18 * jax.random.normal(key_list[6], (LAYERS, C), jnp.float32), 0.1, 1.9)
    chan_bias = centred(key_list[7], (LAYERS, C), 0.5, 3.0, ((1, 16),), jnp.float32)
    w_out = centred(key_list[8], (LAYERS, C, D), C ** -0.5, 0.125, ((1, 32), (2, 16)))
    return dict(tokens=tokens, norm_gain=norm_gain, w_value=w_value, w_gate=w_gate, conv_taps=conv_taps, conv_bias=conv_bias, chan_gain=chan_gain, chan_bias=chan_bias, w_out=w_out)


def reference(tokens, norm_gain, w_value, w_gate, conv_taps, conv_bias, chan_gain, chan_bias, w_out):
    stream = tokens
    rows_total = tokens.shape[0]
    for layer_index in range(LAYERS):
        widened = stream.astype(jnp.float32)
        scale = lax.rsqrt(lax.optimization_barrier(jnp.mean(widened * widened, axis=1, keepdims=True)) + 1e-06)
        normed = (widened * scale * norm_gain[layer_index][None, :]).astype(jnp.bfloat16)
        value = jnp.dot(normed, w_value[layer_index], preferred_element_type=jnp.float32)
        gate = jnp.dot(normed, w_gate[layer_index], preferred_element_type=jnp.float32)
        gated = (value * jax.nn.sigmoid(gate)).astype(jnp.bfloat16)
        padded = jnp.pad(gated.astype(jnp.float32), ((K - 1, 0), (0, 0)))
        convolved = jnp.zeros(gated.shape, jnp.float32) + conv_bias[layer_index][None, :]
        for tap_index in range(K):
            convolved = convolved + conv_taps[layer_index, tap_index][None, :] * padded[tap_index:tap_index + rows_total]
        center = lax.optimization_barrier(jnp.mean(convolved, axis=1, keepdims=True))
        meansq = lax.optimization_barrier(jnp.mean(convolved * convolved, axis=1, keepdims=True))
        spread = meansq - center * center
        shaped = (convolved - center) * lax.rsqrt(spread + 1e-05) * chan_gain[layer_index][None, :] + chan_bias[layer_index][None, :]
        activated = jax.nn.silu(shaped).astype(jnp.bfloat16)
        update = jnp.dot(activated, w_out[layer_index], preferred_element_type=jnp.float32)
        stream = (widened + update).astype(jnp.bfloat16)
    return stream
```

```python
import functools

import jax
import jax.numpy as jnp
from jax import lax
from jax.experimental import pallas as pl
from jax.experimental.pallas import tpu as pltpu
from jax.sharding import Mesh, PartitionSpec as P

F32 = jnp.float32
BF16 = jnp.bfloat16
HALO = 32
VMEM = pl.BlockSpec(memory_space=pltpu.VMEM)
SMEM = pl.BlockSpec(memory_space=pltpu.SMEM)


def parts_of(x):
    high = x.astype(BF16).astype(F32)
    rest = x - high
    middle = rest.astype(BF16).astype(F32)
    return high, middle, (rest - middle).astype(BF16).astype(F32)


def exchanged(x, axis):
    return lax.all_to_all(x, axis, split_axis=0, concat_axis=0, tiled=True)


def shifted(x, axis, steps):
    count = lax.axis_size(axis)
    return lax.ppermute(x, axis, [(i, (i + steps) % count) for i in range(count)])


def row_dot(ones, x):
    return lax.dot_general(
        ones, x, (((1,), (1,)), ((), ())), precision=lax.Precision.HIGHEST, preferred_element_type=F32
    )


def pack_weights(value, gate, out_weights, first, rest):
    deep, depth = value.shape[1], out_weights.shape[1]
    for layer, place in ((0, first), (1, rest)):
        for copy in range(place.shape[0]):
            place[copy, :deep, :128] = value[layer]
            place[copy, :deep, 128:] = gate[layer]
            place[copy, deep : deep + depth, :] = out_weights[layer]
    rest[0, deep + depth :, :] = jnp.zeros((rest.shape[1] - deep - depth, rest.shape[2]), BF16)


def pack_tokens(earlier, tokens, gains, biases, out):
    rows = tokens.shape[0]
    out[:HALO, :] = earlier[...]
    out[HALO : HALO + rows, :] = tokens[...]
    at = lax.broadcasted_iota(jnp.int32, (16, 256), 0)
    tile = jnp.zeros((16, 256), F32)
    for layer in range(2):
        pair = jnp.concatenate([gains[layer : layer + 1, :], biases[layer : layer + 1, :]], axis=1)
        for j, part in enumerate(parts_of(pair)):
            tile = jnp.where(at == 3 * layer + j, part, tile)
    out[HALO + rows :, :] = tile.astype(BF16)


def copy_kernel(x, out):
    for copy in range(out.shape[0]):
        out[copy] = x[:, : out.shape[2], :]


def gated_of(visit, rows, acc, total, squares):
    squares[...] = jnp.zeros(squares.shape, F32)

    def add_squares(block, gain, weights):
        wide = block().astype(F32)
        wide = wide * wide
        squares[...] += wide[:, :128] + wide[:, 128:]

    visit(add_squares)
    scale = lax.rsqrt(jnp.sum(squares[...], axis=1, keepdims=True) / total + 1e-06)
    acc[...] = jnp.zeros(acc.shape, F32)

    def add_product(block, gain, weights):
        normed = (block().astype(F32) * scale * gain()).astype(BF16)
        acc[...] += jnp.dot(normed, weights(), preferred_element_type=F32)

    visit(add_product)
    value = acc[:, :128]
    gate = acc[:, 128:]
    return (value * jax.nn.sigmoid(gate)).astype(BF16)


def convolve_and_pack(extended, taps, bias, layer, out, rows):
    kernel = taps.shape[1]
    convolved = jnp.zeros((rows, 128), F32) + bias[layer : layer + 1, :]
    for k in range(kernel):
        convolved = convolved + taps[layer, k : k + 1, :] * extended[pl.ds(HALO - kernel + 1 + k, rows), :]
    mean = jnp.sum(convolved, axis=1, keepdims=True) * (1.0 / 128.0)
    less = convolved - mean
    ones = jnp.ones((8, 128), F32)
    mean_row = row_dot(ones, convolved) * (1.0 / 128.0)
    square_row = row_dot(ones, less * less)
    at = lax.broadcasted_iota(jnp.int32, (8, 128), 0)
    packed = []
    for row in (mean_row, square_row):
        tile = jnp.zeros((8, 128), F32)
        for j, part in enumerate(parts_of(row)):
            for half in range(2):
                tile = jnp.where(at == 2 * j + half, part[:, half * 128 : half * 128 + 128], tile)
        packed.append(tile)
    small = jnp.concatenate(packed, axis=0).astype(BF16)
    less = less.astype(BF16)
    for copy in range(out.shape[0]):
        out[copy, :rows, :] = less
        out[copy, rows:, :] = small


def first_kernel(rows, tokens, gains, weights, taps, bias, out, acc, squares, extended):
    total = tokens.shape[0] * tokens.shape[2]

    def visit(fn):
        def step(y, carry):
            for c in range(2):
                i = 2 * y + c
                fn(
                    lambda: tokens[i, : HALO + rows, :],
                    lambda: gains[0:1, pl.ds(pl.multiple_of(i * 256, 256), 256)],
                    lambda: jnp.concatenate([weights[2 * c, y], weights[2 * c + 1, y]], axis=0),
                )
            return carry

        lax.fori_loop(0, tokens.shape[0] // 2, step, 0)

    extended[...] = gated_of(visit, rows, acc, total, squares).astype(F32)
    convolve_and_pack(extended, taps, bias, 0, out, rows)


def gate_kernel(core, own, other, gains, weights, out, acc, squares):
    total = 2 * own.shape[0] * own.shape[2]
    here = core[0]

    def visit(fn):
        def step(y, carry):
            for blocks, c in ((own, here), (other, 1 - here)):
                fn(
                    lambda: blocks[y],
                    lambda: gains[1:2, pl.ds(pl.multiple_of((2 * y + c) * 256, 256), 256)],
                    lambda: jnp.concatenate([weights[2 * c, y], weights[2 * c + 1, y]], axis=0),
                )
            return carry

        lax.fori_loop(0, own.shape[0], step, 0)

    out[...] = gated_of(visit, own.shape[1], acc, total, squares)


def conv_kernel(rows, earlier, gated, taps, bias, out, extended):
    extended[:HALO, :] = earlier[...].astype(F32)
    extended[HALO:, :] = gated[...].astype(F32)
    convolve_and_pack(extended, taps, bias, 1, out, rows)


def out_kernel(rows, layer, pieces, place, own, other, params, stream, *rest):
    weights, (out, joined, acc, sides) = rest[:-4], rest[-4:]
    core, across = place[0], place[1]
    count = own.shape[0]
    total = 2 * count * 128

    def stat(tile):
        sums = []
        for half in range(2):
            sums.append(sum(tile[2 * j + half : 2 * j + half + 1, :] for j in range(3)))
        return jnp.concatenate(sums, axis=1)

    means, squares = [], []
    for blocks in (own, other):
        for y in range(count):
            tile = blocks[y, rows:, :].astype(F32)
            means.append(stat(tile[:8]))
            squares.append(stat(tile[8:]))
    means = jnp.concatenate(means, axis=0)
    squares = jnp.concatenate(squares, axis=0)
    center = jnp.mean(means, axis=0, keepdims=True)
    apart = means - center
    spread = jnp.sum(squares + 128.0 * apart * apart, axis=0, keepdims=True) / total
    factor = lax.rsqrt(spread + 1e-05)
    lines = jnp.concatenate([apart * factor, factor, jnp.zeros((128 - 2 * count - 1, rows), F32)], axis=0)
    sides[...] = lines.T

    depth = 64
    if pieces:
        for steps, piece in enumerate(weights):
            source = lax.rem(across + 4 - steps, 4)
            c, h = source // 2, lax.rem(source, 2)
            start = pl.multiple_of(h * depth, depth)
            for y in range(count):
                joined[c, y, pl.ds(start, depth), :] = piece[y]
    else:
        for c in range(2):
            for h in range(2):
                for y in range(count):
                    joined[c, y, h * depth : (h + 1) * depth, :] = weights[0][2 * c + h, y]

    acc[...] = stream[...].astype(F32)
    wide = jnp.broadcast_to(sides[:, 2 * count : 2 * count + 1], (rows, 128))
    for n, (blocks, c) in enumerate(((own, core), (other, 1 - core))):
        for y in range(count):
            param = params[2 * y + c].astype(F32)
            gain, bias = (
                sum(param[3 * layer + j : 3 * layer + j + 1, k * 128 : k * 128 + 128] for j in range(3))
                for k in range(2)
            )
            side = sides[:, n * count + y : n * count + y + 1]
            shaped = (blocks[y, :rows, :].astype(F32) * wide + side) * gain + bias
            activated = (shaped * jax.nn.sigmoid(shaped)).astype(BF16)
            acc[...] += jnp.dot(activated, joined[c, y], preferred_element_type=F32)
    result = acc[...].astype(BF16)
    if len(out.shape) == 2:
        out[...] = result
    else:
        for copy in range(out.shape[0]):
            out[copy] = result


def call(body, shape, name, arrays, scratch=(), scalars=0, flops=1_000_000_000):
    return pl.pallas_call(
        body,
        out_shape=shape,
        in_specs=[SMEM] * scalars + [VMEM] * arrays,
        out_specs=jax.tree.map(lambda _: VMEM, shape),
        scratch_shapes=list(scratch),
        cost_estimate=pl.CostEstimate(flops=flops, bytes_accessed=1_000_000, transcendentals=0),
        compiler_params=pltpu.CompilerParams(vmem_limit_bytes=16 * 1024 * 1024),
        name=name,
    )


def shards(tokens, norm_gain, w_value, w_gate, conv_taps, conv_bias, chan_gain, chan_bias, w_out):
    rows, width = tokens.shape
    ring = lax.axis_size("y")
    line = 2 * ring
    here = lax.axis_index("c").astype(jnp.int32)
    across = lax.axis_index("x").astype(jnp.int32)
    place = jnp.stack([here, across])
    blocks = lax.axis_size("z") * lax.axis_size("x")
    onward = [(i, i + 1) for i in range(blocks - 1)]

    deep, depth = w_value.shape[1], w_out.shape[1]
    first, rest = call(
        pack_weights,
        (
            jax.ShapeDtypeStruct((lax.axis_size("z"), deep + depth, width), BF16),
            jax.ShapeDtypeStruct((1, deep + 2 * depth, width), BF16),
        ),
        "pack_weights",
        3,
    )(w_value, w_gate, w_out)
    first = exchanged(first, "z")
    in_first = call(
        copy_kernel, jax.ShapeDtypeStruct((lax.axis_size("x"), lax.axis_size("z"), deep, width), BF16), "copies", 1
    )(first)
    in_first = exchanged(in_first, "x")
    out_piece = first[:, deep:]

    earlier = lax.ppermute(tokens[rows - HALO :], ("z", "x"), onward)
    packed = call(pack_tokens, jax.ShapeDtypeStruct((HALO + rows + 16, width), BF16), "pack_tokens", 4)(
        earlier, tokens, chan_gain, chan_bias
    )
    everything = lax.all_gather(packed, ("y", "c"))
    params = everything[:, HALO + rows :]

    rest, _ = lax.optimization_barrier((rest[0], everything[0, 0, 0]))
    second = lax.all_gather(rest, "z")
    in_second = lax.all_gather(second[:, :deep], "x")
    out_second = second[:, deep : deep + depth]
    out_second, _ = lax.optimization_barrier((out_second, in_second[0, 0, 0, 0]))
    out_second = lax.all_gather(out_second, "x")

    packed_shape = jax.ShapeDtypeStruct((ring, rows + 16, 128), BF16)
    packed = call(
        functools.partial(first_kernel, rows),
        packed_shape,
        "first",
        5,
        scratch=[
            pltpu.VMEM((HALO + rows, 256), F32),
            pltpu.VMEM((HALO + rows, 128), F32),
            pltpu.VMEM((HALO + rows, 128), F32),
        ],
        flops=4_000_000_000,
    )(everything, norm_gain, in_first, conv_taps, conv_bias)

    def out_step(packed, stream, layer, weights, copies):
        own = exchanged(packed, "y")
        other = shifted(own, "c", 1)
        return call(
            functools.partial(out_kernel, rows, layer, len(weights) > 1),
            jax.ShapeDtypeStruct((copies, rows, width) if copies else (rows, width), BF16),
            "out",
            4 + len(weights),
            scratch=[
                pltpu.VMEM((2, ring, 128, width), BF16),
                pltpu.VMEM((rows, width), F32),
                pltpu.VMEM((rows, 128), F32),
            ],
            scalars=1,
            flops=4_000_000_000,
        )(place, own, other, params, stream, *weights)

    pieces = [out_piece] + [shifted(out_piece, "x", steps) for steps in (1, 2, 3)]
    copies = out_step(packed, tokens, 0, pieces, ring)
    own = exchanged(copies, "y")
    other = shifted(own, "c", 1)
    gated = call(
        gate_kernel,
        jax.ShapeDtypeStruct((rows, 128), BF16),
        "gate",
        4,
        scratch=[pltpu.VMEM((rows, 256), F32), pltpu.VMEM((rows, 128), F32)],
        scalars=1,
        flops=4_000_000_000,
    )(place, own, other, norm_gain, in_second)
    earlier = lax.ppermute(gated[rows - HALO :], ("z", "x"), onward)
    packed = call(
        functools.partial(conv_kernel, rows),
        packed_shape,
        "conv",
        4,
        scratch=[pltpu.VMEM((HALO + rows, 128), F32)],
    )(earlier, gated, conv_taps, conv_bias)
    return out_step(packed, copies[0], 1, [out_second], 0)


def solution(mesh):
    grid = Mesh(mesh.devices.reshape(8, 4, 8, 2), ("z", "x", "y", "c"))
    sp, tp = ("z", "x"), ("y", "c")
    placed = (
        P(sp, tp),
        P(),
        P(None, sp, tp),
        P(None, sp, tp),
        P(None, None, tp),
        P(None, tp),
        P(None, tp),
        P(None, tp),
        P(None, sp, tp),
    )
    return jax.shard_map(shards, mesh=grid, in_specs=placed, out_specs=P(sp, tp), check_vma=False)
```

```python
import functools

import jax
import jax.numpy as jnp
from jax import lax
from jax.experimental import pallas as pl
from jax.experimental.pallas import tpu as pltpu
from jax.sharding import Mesh, PartitionSpec as P


F32 = jnp.float32
BF16 = jnp.bfloat16
HALO = 32
FROM = ((0, 3, -2), (1, 4), (-1, 2, -3))
HBM = pl.BlockSpec(memory_space=pltpu.HBM)
VMEM = pl.BlockSpec(memory_space=pltpu.VMEM)
SMEM = pl.BlockSpec(memory_space=pltpu.SMEM)


def parts_of(x):
    high = x.astype(BF16).astype(F32)
    rest = x - high
    middle = rest.astype(BF16).astype(F32)
    return high, middle, (rest - middle).astype(BF16).astype(F32)


def exchanged(x, axis):
    return lax.all_to_all(x, axis, split_axis=0, concat_axis=0, tiled=True)


def shifted(x, axis, steps):
    count = lax.axis_size(axis)
    return lax.ppermute(x, axis, [(i, (i + steps) % count) for i in range(count)])


def row_dot(ones, x):
    return lax.dot_general(
        ones, x, (((1,), (1,)), ((), ())), precision=lax.Precision.HIGHEST, preferred_element_type=F32
    )


def pack_weights(value, gate, out_weights, first, rest):
    deep, depth = value.shape[1], out_weights.shape[1]
    for copy in range(first.shape[0]):
        first[copy, :, :128] = value[0]
        first[copy, :, 128:] = gate[0]
    rest[:deep, :128] = value[1]
    rest[:deep, 128:] = gate[1]
    rest[deep : deep + depth, :] = out_weights[0]
    rest[deep + depth :, :] = out_weights[1]


def group_kernel(own, third, second, two, three):
    for out in (two, three):
        out[0] = own[...]
        out[1] = third[...]
    three[2] = second[...]


def pack_tokens(earlier, tokens, gains, biases, out, near_gains, near_biases, done):
    rows = tokens.shape[0]
    moves = [
        pltpu.make_async_copy(tokens, out.at[pl.ds(HALO, rows), :], done.at[0]),
        pltpu.make_async_copy(gains, near_gains, done.at[1]),
        pltpu.make_async_copy(biases, near_biases, done.at[2]),
    ]
    for move in moves:
        move.start()
    out[:HALO, :] = earlier[...]
    at = lax.broadcasted_iota(jnp.int32, (16, 256), 0)
    tile = jnp.zeros((16, 256), F32)
    for move in moves:
        move.wait()
    for layer in range(2):
        pair = jnp.concatenate([near_gains[layer : layer + 1, :], near_biases[layer : layer + 1, :]], axis=1)
        for j, part in enumerate(parts_of(pair)):
            tile = jnp.where(at == 3 * layer + j, part, tile)
    out[HALO + rows :, :] = tile.astype(BF16)


def stack_kernel(place, three, ahead, behind, deep, out_first, out_second):
    rows, depth = deep.shape[1], out_first.shape[1]
    for group, steps in zip((three, ahead, behind), FROM, strict=True):
        for j, step in enumerate(steps):
            z = lax.rem(place[2] + 8 - step, 8)
            deep[z] = group[j, :rows, :]
            out_first[z] = group[j, rows : rows + depth, :]
            out_second[z] = group[j, rows + depth :, :]


def join_pieces(place, *refs):
    pieces, out = refs[:-1], refs[-1]
    depth = pieces[0].shape[1]
    for steps, piece in enumerate(pieces):
        source = lax.rem(place[1] + 4 - steps, 4)
        start = pl.multiple_of(lax.rem(source, 2) * depth, depth)
        for y in range(piece.shape[0]):
            out[source // 2, y, pl.ds(start, depth), :] = piece[y]


def join_gathered(weights, out):
    depth = weights.shape[2]
    for c in range(2):
        for h in range(2):
            for y in range(weights.shape[1]):
                out[c, y, h * depth : (h + 1) * depth, :] = weights[2 * c + h, y]


def copy_kernel(x, out):
    for copy in range(out.shape[0]):
        out[copy] = x[:, : out.shape[2], :]


def gated_of(visit, acc, total, squares):
    squares[...] = jnp.zeros(squares.shape, F32)

    def add_squares(block, gain, weights):
        wide = block().astype(F32)
        wide = wide * wide
        squares[...] += wide[:, :128] + wide[:, 128:]

    visit(add_squares)
    scale = lax.rsqrt(jnp.sum(squares[...], axis=1, keepdims=True) / total + 1e-06)
    acc[...] = jnp.zeros(acc.shape, F32)

    def add_product(block, gain, weights):
        normed = (block().astype(F32) * scale * gain()).astype(BF16)
        acc[...] += jnp.dot(normed, weights(), preferred_element_type=F32)

    visit(add_product)
    value = acc[:, :128]
    gate = acc[:, 128:]
    return (value * jax.nn.sigmoid(gate)).astype(BF16)


def convolve_and_pack(extended, taps, bias, layer, out, rows):
    kernel = taps.shape[1]
    convolved = jnp.zeros((rows, 128), F32) + bias[layer : layer + 1, :]
    for k in range(kernel):
        convolved = convolved + taps[layer, k : k + 1, :] * extended[pl.ds(HALO - kernel + 1 + k, rows), :]
    mean = jnp.sum(convolved, axis=1, keepdims=True) * (1.0 / 128.0)
    less = convolved - mean
    ones = jnp.ones((8, 128), F32)
    mean_row = row_dot(ones, convolved) * (1.0 / 128.0)
    square_row = row_dot(ones, less * less)
    at = lax.broadcasted_iota(jnp.int32, (8, 128), 0)
    packed = []
    for row in (mean_row, square_row):
        tile = jnp.zeros((8, 128), F32)
        for j, part in enumerate(parts_of(row)):
            for half in range(2):
                tile = jnp.where(at == 2 * j + half, part[:, half * 128 : half * 128 + 128], tile)
        packed.append(tile)
    small = jnp.concatenate(packed, axis=0).astype(BF16)
    less = less.astype(BF16)
    for copy in range(out.shape[0]):
        out[copy, :rows, :] = less
        out[copy, rows:, :] = small


def first_kernel(rows, tokens, gains, weights, taps, bias, out, acc, squares, extended):
    total = tokens.shape[0] * tokens.shape[2]

    def visit(fn):
        def step(y, carry):
            for c in range(2):
                i = 2 * y + c
                fn(
                    lambda: tokens[i, : HALO + rows, :],
                    lambda: gains[0:1, pl.ds(pl.multiple_of(i * 256, 256), 256)],
                    lambda: jnp.concatenate([weights[2 * c, y], weights[2 * c + 1, y]], axis=0),
                )
            return carry

        lax.fori_loop(0, tokens.shape[0] // 2, step, 0)

    extended[...] = gated_of(visit, acc, total, squares).astype(F32)
    convolve_and_pack(extended, taps, bias, 0, out, rows)


def product_step(block, gain, weights, acc, squares):
    wide = block.astype(F32)
    normed = (wide * gain).astype(BF16)
    wide = wide * wide
    squares[...] += wide[:, :128] + wide[:, 128:]
    acc[...] += jnp.dot(normed, weights, preferred_element_type=F32)


def gate_blocks(groups, place, c, first, gains, weights, acc, squares):
    for blocks, steps in zip(groups, FROM, strict=True):
        for j, step in enumerate(steps):
            y = lax.rem(place[3] + 8 - step, 8)
            gain = gains[1:2, pl.ds(pl.multiple_of((2 * y + c) * 256, 256), 256)]
            depths = jnp.concatenate([weights[2 * c, y], weights[2 * c + 1, y]], axis=0)
            product_step(blocks[j, first:, :], gain, depths, acc, squares)


def gate_own(place, three, ahead, behind, gains, weights, acc, squares):
    acc[...] = jnp.zeros(acc.shape, F32)
    squares[...] = jnp.zeros(squares.shape, F32)
    gate_blocks((three, ahead, behind), place, place[0], 0, gains, weights, acc, squares)


def gate_other(first, place, own_acc, own_squares, three, ahead, behind, gains, weights, out, acc, squares):
    acc[...] = own_acc[first:, :]
    squares[...] = own_squares[first:, :]
    gate_blocks((three, ahead, behind), place, 1 - place[0], first, gains, weights, acc, squares)
    total = 16 * three.shape[2]
    scale = lax.rsqrt(jnp.sum(squares[...], axis=1, keepdims=True) / total + 1e-06)
    value = acc[:, :128] * scale
    gate = acc[:, 128:] * scale
    out[...] = (value * jax.nn.sigmoid(gate)).astype(BF16)


def conv_kernel(rows, earlier, gated, taps, bias, out, extended):
    extended[:HALO, :] = earlier[...].astype(F32)
    extended[HALO:, :] = gated[...].astype(F32)
    convolve_and_pack(extended, taps, bias, 1, out, rows)


def out_kernel(rows, layer, place, own, other, params, stream, joined, out, acc, sides):
    core = place[0]
    count = own.shape[0]
    total = 2 * count * 128

    def stat(tile):
        sums = []
        for half in range(2):
            sums.append(sum(tile[2 * j + half : 2 * j + half + 1, :] for j in range(3)))
        return jnp.concatenate(sums, axis=1)

    means, squares = [], []
    for blocks in (own, other):
        for y in range(count):
            tile = blocks[y, rows:, :].astype(F32)
            means.append(stat(tile[:8]))
            squares.append(stat(tile[8:]))
    means = jnp.concatenate(means, axis=0)
    squares = jnp.concatenate(squares, axis=0)
    center = jnp.mean(means, axis=0, keepdims=True)
    apart = means - center
    spread = jnp.sum(squares + 128.0 * apart * apart, axis=0, keepdims=True) / total
    factor = lax.rsqrt(spread + 1e-05)
    lines = jnp.concatenate([apart * factor, factor, jnp.zeros((128 - 2 * count - 1, rows), F32)], axis=0)
    sides[...] = lines.T

    acc[...] = stream[...].astype(F32)
    wide = jnp.broadcast_to(sides[:, 2 * count : 2 * count + 1], (rows, 128))
    for n, (blocks, c) in enumerate(((own, core), (other, 1 - core))):
        for y in range(count):
            param = params[2 * y + c].astype(F32)
            gain, bias = (
                sum(param[3 * layer + j : 3 * layer + j + 1, k * 128 : k * 128 + 128] for j in range(3))
                for k in range(2)
            )
            side = sides[:, n * count + y : n * count + y + 1]
            shaped = (blocks[y, :rows, :].astype(F32) * wide + side) * gain + bias
            activated = (shaped * jax.nn.sigmoid(shaped)).astype(BF16)
            acc[...] += jnp.dot(activated, joined[c, y], preferred_element_type=F32)
    out[...] = acc[...].astype(BF16)


def call(body, shape, arrays, scratch=(), scalars=0, flops=1_000_000_000, limit=16):
    specs = [VMEM] * arrays if isinstance(arrays, int) else arrays
    return pl.pallas_call(
        body,
        out_shape=shape,
        in_specs=[SMEM] * scalars + specs,
        out_specs=jax.tree.map(lambda _: VMEM, shape),
        scratch_shapes=list(scratch),
        cost_estimate=pl.CostEstimate(flops=flops, bytes_accessed=1_000_000, transcendentals=0),
        compiler_params=pltpu.CompilerParams(vmem_limit_bytes=limit * 1024 * 1024),
    )


def shards(tokens, norm_gain, w_value, w_gate, conv_taps, conv_bias, chan_gain, chan_bias, w_out):
    rows, width = tokens.shape
    ring, deep_ring = lax.axis_size("y"), lax.axis_size("z")
    place = jnp.stack([lax.axis_index(axis).astype(jnp.int32) for axis in ("c", "x", "z", "y")])
    blocks = deep_ring * lax.axis_size("x")
    onward = [(i, i + 1) for i in range(blocks - 1)]
    deep, depth = w_value.shape[1], w_out.shape[1]

    earlier = lax.ppermute(tokens[rows - HALO :], ("z", "x"), onward)
    packed = call(
        pack_tokens,
        jax.ShapeDtypeStruct((HALO + rows + 16, width), BF16),
        [VMEM, HBM, HBM, HBM],
        scratch=[
            pltpu.VMEM(chan_gain.shape, F32),
            pltpu.VMEM(chan_bias.shape, F32),
            pltpu.SemaphoreType.DMA((3,)),
        ],
        limit=60,
    )(earlier, tokens, chan_gain, chan_bias)
    everything = lax.all_gather(packed, ("y", "c"))
    params = everything[:, HALO + rows :]

    def relay(x, axis):
        third, second = shifted(x, axis, 3), shifted(x, axis, -2)
        two, three = call(
            group_kernel, (jax.ShapeDtypeStruct((2, *x.shape), BF16), jax.ShapeDtypeStruct((3, *x.shape), BF16)), 3
        )(x, third, second)
        return three, shifted(two, axis, 1), shifted(three, axis, -1)

    first, rest = call(
        pack_weights,
        (jax.ShapeDtypeStruct((deep_ring, deep, width), BF16), jax.ShapeDtypeStruct((deep + 2 * depth, width), BF16)),
        3,
    )(w_value, w_gate, w_out)
    first = exchanged(first, "z")
    in_first = call(copy_kernel, jax.ShapeDtypeStruct((lax.axis_size("x"), deep_ring, deep, width), BF16), 1)(first)
    in_first = exchanged(in_first, "x")
    groups = relay(rest, "z")
    out_shape = jax.ShapeDtypeStruct((deep_ring, depth, width), BF16)
    in_second, out_first, out_second = call(
        stack_kernel, (jax.ShapeDtypeStruct((deep_ring, deep, width), BF16), out_shape, out_shape), 3, scalars=1
    )(place, *groups)
    joined_shape = jax.ShapeDtypeStruct((2, deep_ring, 2 * depth, width), BF16)
    pieces = [shifted(out_first, "x", steps) for steps in (1, 2, 3)]
    joined_first = call(join_pieces, joined_shape, 4, scalars=1)(place, out_first, *pieces)
    in_second = lax.all_gather(in_second, "x")
    out_second = lax.all_gather(out_second, "x")
    joined_second = call(join_gathered, joined_shape, 1)(out_second)

    packed_shape = jax.ShapeDtypeStruct((ring, rows + 16, 128), BF16)
    packed = call(
        functools.partial(first_kernel, rows),
        packed_shape,
        5,
        scratch=[
            pltpu.VMEM((HALO + rows, 256), F32),
            pltpu.VMEM((HALO + rows, 128), F32),
            pltpu.VMEM((HALO + rows, 128), F32),
        ],
        flops=4_000_000_000,
    )(everything, norm_gain, in_first, conv_taps, conv_bias)

    def out_step(own, other, stream, layer, joined):
        return call(
            functools.partial(out_kernel, rows, layer),
            jax.ShapeDtypeStruct((rows, width), BF16),
            5,
            scratch=[pltpu.VMEM((rows, width), F32), pltpu.VMEM((rows, 128), F32)],
            scalars=1,
            flops=4_000_000_000,
        )(place, own, other, params, stream, joined)

    own = exchanged(packed, "y")
    other = shifted(own, "c", 1)
    stream = out_step(own, other, tokens, 0, joined_first)
    own = relay(stream, "y")
    other = [shifted(group, "c", 1) for group in own]
    sums = (jax.ShapeDtypeStruct((rows, 256), F32), jax.ShapeDtypeStruct((rows, 128), F32))
    acc, squares = call(gate_own, sums, 5, scalars=1, flops=4_000_000_000)(place, *own, norm_gain, in_second)

    def gate_rest(first):
        return call(
            functools.partial(gate_other, first),
            jax.ShapeDtypeStruct((rows - first, 128), BF16),
            7,
            scratch=[pltpu.VMEM((rows - first, 256), F32), pltpu.VMEM((rows - first, 128), F32)],
            scalars=1,
            flops=4_000_000_000,
        )(place, acc, squares, *other, norm_gain, in_second)

    last = gate_rest(rows - HALO)
    earlier = lax.ppermute(last, ("z", "x"), onward)
    gated = gate_rest(0)
    packed = call(
        functools.partial(conv_kernel, rows), packed_shape, 4, scratch=[pltpu.VMEM((HALO + rows, 128), F32)]
    )(earlier, gated, conv_taps, conv_bias)
    own = exchanged(packed, "y")
    other = shifted(own, "c", 1)
    return out_step(own, other, stream, 1, joined_second)


def solution(mesh):
    grid = Mesh(mesh.devices.reshape(8, 4, 8, 2), ("z", "x", "y", "c"))
    sp, tp = ("z", "x"), ("y", "c")
    placed = (
        P(sp, tp),
        P(),
        P(None, sp, tp),
        P(None, sp, tp),
        P(None, None, tp),
        P(None, tp),
        P(None, tp),
        P(None, tp),
        P(None, sp, tp),
    )
    return jax.shard_map(shards, mesh=grid, in_specs=placed, out_specs=P(sp, tp), check_vma=False)
```

```python
import functools

import jax
import jax.numpy as jnp
from jax import lax
from jax.experimental import pallas as pl
from jax.experimental.pallas import tpu as pltpu
from jax.sharding import Mesh, PartitionSpec as P


F32 = jnp.float32
BF16 = jnp.bfloat16
HALO = 32
FROM = ((0, 3, -2), (1, 4), (-1, 2, -3))
HBM = pl.BlockSpec(memory_space=pltpu.HBM)
VMEM = pl.BlockSpec(memory_space=pltpu.VMEM)
SMEM = pl.BlockSpec(memory_space=pltpu.SMEM)


def parts_of(x):
    high = x.astype(BF16).astype(F32)
    rest = x - high
    middle = rest.astype(BF16).astype(F32)
    return high, middle, (rest - middle).astype(BF16).astype(F32)


def exchanged(x, axis):
    return lax.all_to_all(x, axis, split_axis=0, concat_axis=0, tiled=True)


def shifted(x, axis, steps):
    count = lax.axis_size(axis)
    return lax.ppermute(x, axis, [(i, (i + steps) % count) for i in range(count)])


def row_dot(ones, x):
    return lax.dot_general(
        ones, x, (((1,), (1,)), ((), ())), precision=lax.Precision.HIGHEST, preferred_element_type=F32
    )


def pack_weights(value, gate, out_weights, first, rest):
    deep, depth = value.shape[1], out_weights.shape[1]
    for copy in range(first.shape[0]):
        first[copy, :, :128] = value[0]
        first[copy, :, 128:] = gate[0]
    rest[:deep, :128] = value[1]
    rest[:deep, 128:] = gate[1]
    rest[deep : deep + depth, :] = out_weights[1]
    rest[deep + depth :, :] = out_weights[0]


def group_kernel(own, third, second, *outs):
    start = 0
    for two, three in zip(outs[::2], outs[1::2], strict=True):
        rows = slice(start, start + two.shape[1])
        for out in (two, three):
            out[0] = own[rows, :]
            out[1] = third[rows, :]
        three[2] = second[rows, :]
        start += two.shape[1]


def pack_tokens(tokens, gains, biases, out, near_gains, near_biases, done):
    rows = tokens.shape[0]
    moves = [
        pltpu.make_async_copy(tokens, out.at[pl.ds(0, rows), :], done.at[0]),
        pltpu.make_async_copy(gains, near_gains, done.at[1]),
        pltpu.make_async_copy(biases, near_biases, done.at[2]),
    ]
    for move in moves:
        move.start()
    at = lax.broadcasted_iota(jnp.int32, (16, 256), 0)
    tile = jnp.zeros((16, 256), F32)
    for move in moves:
        move.wait()
    for layer in range(2):
        pair = jnp.concatenate([near_gains[layer : layer + 1, :], near_biases[layer : layer + 1, :]], axis=1)
        for j, part in enumerate(parts_of(pair)):
            tile = jnp.where(at == 3 * layer + j, part, tile)
    out[rows:, :] = tile.astype(BF16)


def stack_kernel(parts, place, three, ahead, behind, *outs):
    for group, steps in zip((three, ahead, behind), FROM, strict=True):
        for j, step in enumerate(steps):
            z = lax.rem(place[2] + 8 - step, 8)
            for (start, stop), out in zip(parts, outs, strict=True):
                out[z] = group[j, start:stop, :]


def join_gathered(weights, joined):
    depth = weights.shape[2]
    for c in range(2):
        for h in range(2):
            for y in range(weights.shape[1]):
                joined[c, y, h * depth : (h + 1) * depth, :] = weights[2 * c + h, y]


def copy_kernel(x, out, done):
    moves = [pltpu.make_async_copy(x, out.at[copy], done.at[copy]) for copy in range(out.shape[0])]
    for move in moves:
        move.start()
    for move in moves:
        move.wait()


def convolve_and_pack(extended, taps, bias, layer, out, rows):
    kernel = taps.shape[1]
    convolved = jnp.zeros((rows, 128), F32) + bias[layer : layer + 1, :]
    for k in range(kernel):
        convolved = convolved + taps[layer, k : k + 1, :] * extended[pl.ds(HALO - kernel + 1 + k, rows), :]
    mean = jnp.sum(convolved, axis=1, keepdims=True) * (1.0 / 128.0)
    less = convolved - mean
    ones = jnp.ones((8, 128), F32)
    mean_row = row_dot(ones, convolved) * (1.0 / 128.0)
    square_row = row_dot(ones, less * less)
    at = lax.broadcasted_iota(jnp.int32, (8, 128), 0)
    packed = []
    for row in (mean_row, square_row):
        tile = jnp.zeros((8, 128), F32)
        for j, part in enumerate(parts_of(row)):
            for half in range(2):
                tile = jnp.where(at == 2 * j + half, part[:, half * 128 : half * 128 + 128], tile)
        packed.append(tile)
    small = jnp.concatenate(packed, axis=0).astype(BF16)
    less = less.astype(BF16)
    for copy in range(out.shape[0]):
        out[copy, :rows, :] = less
        out[copy, rows:, :] = small


def gated_from(acc, squares, total):
    scale = lax.rsqrt(jnp.sum(squares, axis=1, keepdims=True) / total + 1e-06)
    value = acc[:, :128] * scale
    gate = acc[:, 128:] * scale
    return value * jax.nn.sigmoid(gate)


def first_gate(tokens, gains, weights, out, acc, squares):
    rows = out.shape[0]
    acc[...] = jnp.zeros(acc.shape, F32)
    squares[...] = jnp.zeros(squares.shape, F32)
    for i in range(tokens.shape[0]):
        y, c = divmod(i, 2)
        gain = gains[0:1, i * 256 : i * 256 + 256]
        depths = jnp.concatenate([weights[2 * c, y], weights[2 * c + 1, y]], axis=0)
        product_step(tokens[i, :rows, :], gain, depths, acc, squares)
    out[...] = gated_from(acc, squares[...], tokens.shape[0] * tokens.shape[2]).astype(BF16)


def product_step(block, gain, weights, acc, squares):
    wide = block.astype(F32)
    normed = (wide * gain).astype(BF16)
    wide = wide * wide
    squares[...] += wide[:, :128] + wide[:, 128:]
    acc[...] += jnp.dot(normed, weights, preferred_element_type=F32)


def gate_blocks(blocks, c, first, gains, weights, acc, squares):
    for y in range(blocks.shape[0]):
        gain = gains[1:2, pl.ds(pl.multiple_of((2 * y + c) * 256, 256), 256)]
        depths = jnp.concatenate([weights[2 * c, y], weights[2 * c + 1, y]], axis=0)
        product_step(blocks[y, first:, :], gain, depths, acc, squares)


def gate_own(place, own, gains, weights, acc, squares):
    acc[...] = jnp.zeros(acc.shape, F32)
    squares[...] = jnp.zeros(squares.shape, F32)
    gate_blocks(own, place[0], 0, gains, weights, acc, squares)


def gate_other(place, own_acc, own_squares, other, gains, weights, out, acc, squares):
    first = own_acc.shape[0] - out.shape[0]
    acc[...] = own_acc[first:, :]
    squares[...] = own_squares[first:, :]
    gate_blocks(other, 1 - place[0], first, gains, weights, acc, squares)
    out[...] = gated_from(acc, squares[...], 2 * other.shape[0] * other.shape[2]).astype(BF16)


def conv_kernel(rows, layer, earlier, gated, taps, bias, out, extended):
    extended[:HALO, :] = earlier[...].astype(F32)
    extended[HALO:, :] = gated[...].astype(F32)
    convolve_and_pack(extended, taps, bias, layer, out, rows)


def out_kernel(rows, layer, place, own, other, params, stream, joined, out, acc, sides):
    core = place[0]
    count = own.shape[0]
    total = 2 * count * 128

    def stat(tile):
        sums = []
        for half in range(2):
            sums.append(sum(tile[2 * j + half : 2 * j + half + 1, :] for j in range(3)))
        return jnp.concatenate(sums, axis=1)

    means, squares = [], []
    for blocks in (own, other):
        for y in range(count):
            tile = blocks[y, rows:, :].astype(F32)
            means.append(stat(tile[:8]))
            squares.append(stat(tile[8:]))
    means = jnp.concatenate(means, axis=0)
    squares = jnp.concatenate(squares, axis=0)
    center = jnp.mean(means, axis=0, keepdims=True)
    apart = means - center
    spread = jnp.sum(squares + 128.0 * apart * apart, axis=0, keepdims=True) / total
    factor = lax.rsqrt(spread + 1e-05)
    lines = jnp.concatenate([apart * factor, factor, jnp.zeros((128 - 2 * count - 1, rows), F32)], axis=0)
    sides[...] = lines.T

    acc[...] = stream[...].astype(F32)
    wide = jnp.broadcast_to(sides[:, 2 * count : 2 * count + 1], (rows, 128))
    for n, (blocks, c) in enumerate(((own, core), (other, 1 - core))):
        for y in range(count):
            param = params[2 * y + c].astype(F32)
            gain, bias = (
                sum(param[3 * layer + j : 3 * layer + j + 1, k * 128 : k * 128 + 128] for j in range(3))
                for k in range(2)
            )
            side = sides[:, n * count + y : n * count + y + 1]
            shaped = (blocks[y, :rows, :].astype(F32) * wide + side) * gain + bias
            activated = (shaped * jax.nn.sigmoid(shaped)).astype(BF16)
            acc[...] += jnp.dot(activated, joined[c, y], preferred_element_type=F32)
    result = acc[...].astype(BF16)
    if len(out.shape) == 2:
        out[...] = result
    else:
        for copy in range(out.shape[0]):
            out[copy] = result


def call(body, shape, arrays, scratch=(), scalars=0, flops=1_000_000_000, limit=8, into=VMEM):
    specs = [VMEM] * arrays if isinstance(arrays, int) else arrays
    return pl.pallas_call(
        body,
        out_shape=shape,
        in_specs=[SMEM] * scalars + specs,
        out_specs=jax.tree.map(lambda _: into, shape),
        scratch_shapes=list(scratch),
        cost_estimate=pl.CostEstimate(flops=flops, bytes_accessed=1_000_000, transcendentals=0),
        compiler_params=pltpu.CompilerParams(vmem_limit_bytes=limit * 1024 * 1024),
    )


def shards(tokens, norm_gain, w_value, w_gate, conv_taps, conv_bias, chan_gain, chan_bias, w_out):
    rows, width = tokens.shape
    ring, deep_ring = lax.axis_size("y"), lax.axis_size("z")
    place = jnp.stack([lax.axis_index(axis).astype(jnp.int32) for axis in ("c", "x", "z", "y")])
    blocks = deep_ring * lax.axis_size("x")
    onward = [(i, i + 1) for i in range(blocks - 1)]
    deep, depth = w_value.shape[1], w_out.shape[1]

    packed = call(
        pack_tokens,
        jax.ShapeDtypeStruct((rows + 16, width), BF16),
        [HBM, HBM, HBM],
        scratch=[
            pltpu.VMEM(chan_gain.shape, F32),
            pltpu.VMEM(chan_bias.shape, F32),
            pltpu.SemaphoreType.DMA((3,)),
        ],
        limit=60,
    )(tokens, chan_gain, chan_bias)
    everything = lax.all_gather(packed, ("y", "c"))
    params = everything[:, rows:]

    def relay(x, axis, cuts):
        third, second = shifted(x, axis, 3), shifted(x, axis, -2)
        shapes = [jax.ShapeDtypeStruct((count, cut, width), BF16) for cut in cuts for count in (2, 3)]
        grouped = call(group_kernel, shapes, 3)(x, third, second)
        groups = []
        for two, three in zip(grouped[::2], grouped[1::2], strict=True):
            groups.append((three, shifted(two, axis, 1), shifted(three, axis, -1)))
        return groups

    first, rest = call(
        pack_weights,
        (jax.ShapeDtypeStruct((deep_ring, deep, width), BF16), jax.ShapeDtypeStruct((deep + 2 * depth, width), BF16)),
        3,
    )(w_value, w_gate, w_out)
    first = exchanged(first, "z")
    across = lax.axis_size("x")
    in_first = call(
        copy_kernel,
        jax.ShapeDtypeStruct((across, deep_ring, deep, width), BF16),
        1,
        scratch=[pltpu.SemaphoreType.DMA((across,))],
        into=HBM,
    )(first)
    in_first = exchanged(in_first, "x")
    late, soon = relay(rest, "z", (deep + depth, depth))

    def stacked(groups, *parts):
        shapes = [jax.ShapeDtypeStruct((deep_ring, stop - start, width), BF16) for start, stop in parts]
        return call(functools.partial(stack_kernel, parts), shapes, 3, scalars=1)(place, *groups)

    (out_first,) = stacked(soon, (0, depth))
    in_second, out_second = stacked(late, (0, deep), (deep, deep + depth))
    out_first = lax.all_gather(out_first, "x")
    in_second = lax.all_gather(in_second, "x")
    out_second = lax.all_gather(out_second, "x")

    def convolved(layer, last, gated):
        earlier = lax.ppermute(last, ("z", "x"), onward)
        return call(
            functools.partial(conv_kernel, rows, layer),
            jax.ShapeDtypeStruct((ring, rows + 16, 128), BF16),
            4,
            scratch=[pltpu.VMEM((HALO + rows, 128), F32)],
        )(earlier, gated, conv_taps, conv_bias)

    def gate(count, body, *arrays, scalars=0):
        return call(
            body,
            jax.ShapeDtypeStruct((count, 128), BF16),
            len(arrays) - scalars,
            scratch=[pltpu.VMEM((count, 256), F32), pltpu.VMEM((count, 128), F32)],
            scalars=scalars,
            flops=4_000_000_000,
        )(*arrays)

    def out_step(own, other, stream, layer, weights, copies):
        joined = call(join_gathered, jax.ShapeDtypeStruct((2, ring, 2 * depth, width), BF16), 1)(weights)
        return call(
            functools.partial(out_kernel, rows, layer),
            jax.ShapeDtypeStruct((copies, rows, width) if copies else (rows, width), BF16),
            5,
            scratch=[pltpu.VMEM((rows, width), F32), pltpu.VMEM((rows, 128), F32)],
            scalars=1,
            flops=4_000_000_000,
        )(place, own, other, params, stream, joined)

    tail = everything[:, rows - HALO : rows]
    last = gate(HALO, first_gate, tail, norm_gain, in_first)
    gated = gate(rows, first_gate, everything, norm_gain, in_first)
    packed = convolved(0, last, gated)
    own = exchanged(packed, "y")
    other = shifted(own, "c", 1)
    copies = out_step(own, other, tokens, 0, out_first, ring)
    own = exchanged(copies, "y")
    other = shifted(own, "c", 1)
    sums = (jax.ShapeDtypeStruct((rows, 256), F32), jax.ShapeDtypeStruct((rows, 128), F32))
    acc, squares = call(gate_own, sums, 3, scalars=1, flops=4_000_000_000)(place, own, norm_gain, in_second)

    rest = (place, acc, squares, other, norm_gain, in_second)
    last = gate(HALO, gate_other, *rest, scalars=1)
    gated = gate(rows, gate_other, *rest, scalars=1)
    packed = convolved(1, last, gated)
    own = exchanged(packed, "y")
    other = shifted(own, "c", 1)
    return out_step(own, other, copies[0], 1, out_second, 0)


def solution(mesh):
    grid = Mesh(mesh.devices.reshape(8, 4, 8, 2), ("z", "x", "y", "c"))
    sp, tp = ("z", "x"), ("y", "c")
    placed = (
        P(sp, tp),
        P(),
        P(None, sp, tp),
        P(None, sp, tp),
        P(None, None, tp),
        P(None, tp),
        P(None, tp),
        P(None, tp),
        P(None, sp, tp),
    )
    return jax.shard_map(shards, mesh=grid, in_specs=placed, out_specs=P(sp, tp), check_vma=False)
```

```python
import functools

import jax
import jax.numpy as jnp
from jax import lax
from jax.experimental import pallas as pl
from jax.experimental.pallas import tpu as pltpu
from jax.sharding import Mesh, PartitionSpec as P


F32 = jnp.float32
BF16 = jnp.bfloat16
HALO = 32
FROM = ((0, 3, -2), (1, 4), (-1, 2, -3))
HBM = pl.BlockSpec(memory_space=pltpu.HBM)
VMEM = pl.BlockSpec(memory_space=pltpu.VMEM)


def parts_of(x):
    high = x.astype(BF16).astype(F32)
    rest = x - high
    middle = rest.astype(BF16).astype(F32)
    return high, middle, (rest - middle).astype(BF16).astype(F32)


def exchanged(x, axis):
    return lax.all_to_all(x, axis, split_axis=0, concat_axis=0, tiled=True)


def shifted(x, axis, steps):
    count = lax.axis_size(axis)
    return lax.ppermute(x, axis, [(i, (i + steps) % count) for i in range(count)])


def row_dot(ones, x):
    return lax.dot_general(
        ones, x, (((1,), (1,)), ((), ())), precision=lax.Precision.HIGHEST, preferred_element_type=F32
    )


def pack_weights(value, gate, out_weights, first, rest):
    deep, depth = value.shape[1], out_weights.shape[1]
    for copy in range(first.shape[0]):
        first[copy, :, :128] = value[0]
        first[copy, :, 128:] = gate[0]
    rest[:deep, :128] = value[1]
    rest[:deep, 128:] = gate[1]
    rest[deep : deep + depth, :] = out_weights[1]
    rest[deep + depth :, :] = out_weights[0]


def group_kernel(own, third, second, *outs):
    start = 0
    for two, three in zip(outs[::2], outs[1::2], strict=True):
        rows = slice(start, start + two.shape[1])
        for out in (two, three):
            out[0] = own[rows, :]
            out[1] = third[rows, :]
        three[2] = second[rows, :]
        start += two.shape[1]


def pack_tokens(tokens, gains, biases, out, near_gains, near_biases, done):
    rows = tokens.shape[0]
    moves = [
        pltpu.make_async_copy(tokens, out.at[pl.ds(0, rows), :], done.at[0]),
        pltpu.make_async_copy(gains, near_gains, done.at[1]),
        pltpu.make_async_copy(biases, near_biases, done.at[2]),
    ]
    for move in moves:
        move.start()
    at = lax.broadcasted_iota(jnp.int32, (16, 256), 0)
    tile = jnp.zeros((16, 256), F32)
    for move in moves:
        move.wait()
    for layer in range(2):
        pair = jnp.concatenate([near_gains[layer : layer + 1, :], near_biases[layer : layer + 1, :]], axis=1)
        for j, part in enumerate(parts_of(pair)):
            tile = jnp.where(at == 3 * layer + j, part, tile)
    out[rows:, :] = tile.astype(BF16)


def stack_kernel(parts, three, ahead, behind, *outs):
    for group, steps in zip((three, ahead, behind), FROM, strict=True):
        for j, step in enumerate(steps):
            z = lax.rem(lax.axis_index("z") + 8 - step, 8)
            for (start, stop), out in zip(parts, outs, strict=True):
                out[z] = group[j, start:stop, :]


def join_gathered(weights, joined):
    depth = weights.shape[2]
    for c in range(2):
        for h in range(2):
            for y in range(weights.shape[1]):
                joined[c, y, h * depth : (h + 1) * depth, :] = weights[2 * c + h, y]


def copy_kernel(x, out, done):
    moves = [pltpu.make_async_copy(x, out.at[copy], done.at[copy]) for copy in range(out.shape[0])]
    for move in moves:
        move.start()
    for move in moves:
        move.wait()


def convolve_and_pack(extended, taps, bias, layer, out, rows):
    kernel = taps.shape[1]
    convolved = jnp.zeros((rows, 128), F32) + bias[layer : layer + 1, :]
    for k in range(kernel):
        convolved = convolved + taps[layer, k : k + 1, :] * extended[pl.ds(HALO - kernel + 1 + k, rows), :]
    mean = jnp.sum(convolved, axis=1, keepdims=True) * (1.0 / 128.0)
    less = convolved - mean
    ones = jnp.ones((8, 128), F32)
    mean_row = row_dot(ones, convolved) * (1.0 / 128.0)
    square_row = row_dot(ones, less * less)
    at = lax.broadcasted_iota(jnp.int32, (8, 128), 0)
    packed = []
    for row in (mean_row, square_row):
        tile = jnp.zeros((8, 128), F32)
        for j, part in enumerate(parts_of(row)):
            for half in range(2):
                tile = jnp.where(at == 2 * j + half, part[:, half * 128 : half * 128 + 128], tile)
        packed.append(tile)
    small = jnp.concatenate(packed, axis=0).astype(BF16)
    less = less.astype(BF16)
    for copy in range(out.shape[0]):
        out[copy, :rows, :] = less
        out[copy, rows:, :] = small


def gated_from(acc, squares, total):
    scale = lax.rsqrt(jnp.sum(squares, axis=1, keepdims=True) / total + 1e-06)
    value = acc[:, :128] * scale
    gate = acc[:, 128:] * scale
    return value * jax.nn.sigmoid(gate)


def first_gate(tokens, gains, weights, out, acc, squares):
    rows = out.shape[0]
    acc[...] = jnp.zeros(acc.shape, F32)
    squares[...] = jnp.zeros(squares.shape, F32)
    for i in range(tokens.shape[0]):
        y, c = divmod(i, 2)
        gain = gains[0:1, i * 256 : i * 256 + 256]
        depths = jnp.concatenate([weights[2 * c, y], weights[2 * c + 1, y]], axis=0)
        product_step(tokens[i, :rows, :], gain, depths, acc, squares)
    out[...] = gated_from(acc, squares[...], tokens.shape[0] * tokens.shape[2]).astype(BF16)


def product_step(block, gain, weights, acc, squares):
    wide = block.astype(F32)
    normed = (wide * gain).astype(BF16)
    wide = wide * wide
    squares[...] += wide[:, :128] + wide[:, 128:]
    acc[...] += jnp.dot(normed, weights, preferred_element_type=F32)


def gate_blocks(blocks, c, first, gains, weights, acc, squares):
    for y in range(blocks.shape[0]):
        gain = gains[1:2, pl.ds(pl.multiple_of((2 * y + c) * 256, 256), 256)]
        depths = jnp.concatenate([weights[2 * c, y], weights[2 * c + 1, y]], axis=0)
        product_step(blocks[y, first:, :], gain, depths, acc, squares)


def gate_own(own, gains, weights, acc, squares):
    acc[...] = jnp.zeros(acc.shape, F32)
    squares[...] = jnp.zeros(squares.shape, F32)
    gate_blocks(own, lax.axis_index("c"), 0, gains, weights, acc, squares)


def gate_other(own_acc, own_squares, other, gains, weights, out, acc, squares):
    first = own_acc.shape[0] - out.shape[0]
    acc[...] = own_acc[first:, :]
    squares[...] = own_squares[first:, :]
    gate_blocks(other, 1 - lax.axis_index("c"), first, gains, weights, acc, squares)
    out[...] = gated_from(acc, squares[...], 2 * other.shape[0] * other.shape[2]).astype(BF16)


def conv_kernel(rows, layer, earlier, gated, taps, bias, out, extended):
    extended[:HALO, :] = earlier[...].astype(F32)
    extended[HALO:, :] = gated[...].astype(F32)
    convolve_and_pack(extended, taps, bias, layer, out, rows)


def out_kernel(rows, layer, own, other, params, stream, joined, *rest):
    core = lax.axis_index("c")
    outs, (acts, sides) = rest[:-2], rest[-2:]
    count = own.shape[0]
    total = 2 * count * 128

    def stat(tile):
        sums = []
        for half in range(2):
            sums.append(sum(tile[2 * j + half : 2 * j + half + 1, :] for j in range(3)))
        return jnp.concatenate(sums, axis=1)

    means, squares = [], []
    for blocks in (own, other):
        for y in range(count):
            tile = blocks[y, rows:, :].astype(F32)
            means.append(stat(tile[:8]))
            squares.append(stat(tile[8:]))
    means = jnp.concatenate(means, axis=0)
    squares = jnp.concatenate(squares, axis=0)
    center = jnp.mean(means, axis=0, keepdims=True)
    apart = means - center
    spread = jnp.sum(squares + 128.0 * apart * apart, axis=0, keepdims=True) / total
    factor = lax.rsqrt(spread + 1e-05)
    lines = jnp.concatenate([apart * factor, factor, jnp.zeros((128 - 2 * count - 1, rows), F32)], axis=0)
    sides[...] = lines.T

    wide = jnp.broadcast_to(sides[:, 2 * count : 2 * count + 1], (rows, 128))
    total = stream[...].astype(F32)
    for n, (blocks, c) in enumerate(((own, core), (other, 1 - core))):
        for y in range(count):
            param = params[2 * y + c].astype(F32)
            gain, bias = (
                sum(param[3 * layer + j : 3 * layer + j + 1, k * 128 : k * 128 + 128] for j in range(3))
                for k in range(2)
            )
            side = sides[:, n * count + y : n * count + y + 1]
            shaped = (blocks[y, :rows, :].astype(F32) * wide + side) * gain + bias
            acts[:, y * 128 : y * 128 + 128] = (shaped * jax.nn.sigmoid(shaped)).astype(BF16)
        weights = joined[c].reshape(count * 128, joined.shape[3])
        total = total + jnp.dot(acts[...], weights, preferred_element_type=F32)
    result = total.astype(BF16)
    outs[0][...] = result
    for out in outs[1:]:
        for copy in range(out.shape[0]):
            out[copy] = result


def call(body, shape, arrays, scratch=(), flops=1_000_000_000, limit=8, into=VMEM):
    specs = [VMEM] * arrays if isinstance(arrays, int) else arrays
    return pl.pallas_call(
        body,
        out_shape=shape,
        in_specs=specs,
        out_specs=jax.tree.map(lambda _: into, shape),
        scratch_shapes=list(scratch),
        cost_estimate=pl.CostEstimate(flops=flops, bytes_accessed=1_000_000, transcendentals=0),
        compiler_params=pltpu.CompilerParams(vmem_limit_bytes=limit * 1024 * 1024),
    )


def shards(tokens, norm_gain, w_value, w_gate, conv_taps, conv_bias, chan_gain, chan_bias, w_out):
    rows, width = tokens.shape
    ring, deep_ring = lax.axis_size("y"), lax.axis_size("z")
    blocks = deep_ring * lax.axis_size("x")
    onward = [(i, i + 1) for i in range(blocks - 1)]
    deep, depth = w_value.shape[1], w_out.shape[1]

    packed = call(
        pack_tokens,
        jax.ShapeDtypeStruct((rows + 16, width), BF16),
        [HBM, HBM, HBM],
        scratch=[
            pltpu.VMEM(chan_gain.shape, F32),
            pltpu.VMEM(chan_bias.shape, F32),
            pltpu.SemaphoreType.DMA((3,)),
        ],
        limit=60,
    )(tokens, chan_gain, chan_bias)
    everything = lax.all_gather(packed, ("y", "c"))
    params = everything[:, rows:]

    def relay(x, axis, cuts):
        third, second = shifted(x, axis, 3), shifted(x, axis, -2)
        shapes = [jax.ShapeDtypeStruct((count, cut, width), BF16) for cut in cuts for count in (2, 3)]
        grouped = call(group_kernel, shapes, 3)(x, third, second)
        groups = []
        for two, three in zip(grouped[::2], grouped[1::2], strict=True):
            behind = shifted(three, axis, -1)
            groups.append((three, shifted(two, axis, 1), behind))
        return groups

    first, rest = call(
        pack_weights,
        (jax.ShapeDtypeStruct((deep_ring, deep, width), BF16), jax.ShapeDtypeStruct((deep + 2 * depth, width), BF16)),
        3,
    )(w_value, w_gate, w_out)
    first = exchanged(first, "z")
    across = lax.axis_size("x")
    in_first = call(
        copy_kernel,
        jax.ShapeDtypeStruct((across, deep_ring, deep, width), BF16),
        1,
        scratch=[pltpu.SemaphoreType.DMA((across,))],
        into=HBM,
    )(first)
    in_first = exchanged(in_first, "x")
    late, soon = relay(rest, "z", (deep + depth, depth))

    def stacked(groups, *parts):
        shapes = [jax.ShapeDtypeStruct((deep_ring, stop - start, width), BF16) for start, stop in parts]
        return call(functools.partial(stack_kernel, parts), shapes, 3)(*groups)

    (out_first,) = stacked(soon, (0, depth))
    (in_second,) = stacked(late, (0, deep))
    (out_second,) = stacked(late, (deep, deep + depth))
    out_first = lax.all_gather(out_first, "x")
    in_second = lax.all_gather(in_second, "x")
    out_second = lax.all_gather(out_second, "x")

    def convolved(layer, last, gated):
        earlier = lax.ppermute(last, ("z", "x"), onward)
        return call(
            functools.partial(conv_kernel, rows, layer),
            jax.ShapeDtypeStruct((ring, rows + 16, 128), BF16),
            4,
            scratch=[pltpu.VMEM((HALO + rows, 128), F32)],
        )(earlier, gated, conv_taps, conv_bias)

    def gate(count, body, *arrays):
        return call(
            body,
            jax.ShapeDtypeStruct((count, 128), BF16),
            len(arrays),
            scratch=[pltpu.VMEM((count, 256), F32), pltpu.VMEM((count, 128), F32)],
            flops=4_000_000_000,
        )(*arrays)

    def out_step(own, other, stream, layer, weights, copies):
        joined = call(join_gathered, jax.ShapeDtypeStruct((2, ring, 2 * depth, width), BF16), 1)(weights)
        return call(
            functools.partial(out_kernel, rows, layer),
            [jax.ShapeDtypeStruct((*count, rows, width), BF16) for count in ((), (copies,))[: 1 + bool(copies)]],
            5,
            scratch=[pltpu.VMEM((rows, ring * 128), BF16), pltpu.VMEM((rows, 128), F32)],
            flops=4_000_000_000,
        )(own, other, params, stream, joined)

    tail = everything[:, rows - HALO : rows]
    last = gate(HALO, first_gate, tail, norm_gain, in_first)
    gated = gate(rows, first_gate, everything, norm_gain, in_first)
    packed = convolved(0, last, gated)
    own = exchanged(packed, "y")
    other = shifted(own, "c", 1)
    stream, copies = out_step(own, other, tokens, 0, out_first, ring)
    own = exchanged(copies, "y")
    other = shifted(own, "c", 1)
    sums = (jax.ShapeDtypeStruct((rows, 256), F32), jax.ShapeDtypeStruct((rows, 128), F32))
    acc, squares = call(gate_own, sums, 3, flops=4_000_000_000)(
        own, norm_gain, in_second
    )

    rest = (acc, squares, other, norm_gain, in_second)
    last = gate(HALO, gate_other, *rest)
    gated = gate(rows, gate_other, *rest)
    packed = convolved(1, last, gated)
    own = exchanged(packed, "y")
    other = shifted(own, "c", 1)
    return out_step(own, other, stream, 1, out_second, 0)[0]


def solution(mesh):
    grid = Mesh(mesh.devices.reshape(8, 4, 8, 2), ("z", "x", "y", "c"))
    sp, tp = ("z", "x"), ("y", "c")
    placed = (
        P(sp, tp),
        P(),
        P(None, sp, tp),
        P(None, sp, tp),
        P(None, None, tp),
        P(None, tp),
        P(None, tp),
        P(None, tp),
        P(None, sp, tp),
    )
    return jax.shard_map(shards, mesh=grid, in_specs=placed, out_specs=P(sp, tp), check_vma=False)
```
